32 devices in a mesh: grp: 2 (over y), kv: 4 (over z), tp: 4 (over x, core).
Axes of the slice: x: 2, y: 2, z: 4, core: 2. Of those that a mesh axis runs over, the one named last changes fastest.
Arguments:
- tokens: bfloat16 [4096, 2048], P(('grp', 'kv'), 'tp'), parts along dimension 0, may hold values from -5400 to 5400, as said below
- gain: bfloat16 [2048], replicated, may hold values from 0.099609375 to 1.8984375
- w_query: bfloat16 [2048, 1024], P(None, 'tp'), may hold values from -1 to 1
- w_key: bfloat16 [2048, 512], P(None, 'tp'), may hold values from -3 to 3
- w_value: bfloat16 [2048, 512], P(None, 'tp'), may hold values from -0.125 to 0.125
- w_out: bfloat16 [1024, 2048], P(None, 'tp'), may hold values from -2 to 2
- select: int32 [32, 32], P(('grp', 'kv')), parts along dimension 0, may hold values from -1 to 63, as said below
Outputs:
- mixed: bfloat16 [4096, 2048], P(('grp', 'kv'), 'tp'), parts along dimension 0
The draws below stay inside these ranges and needn't reach their ends.
There are 2 independent parts, one for each index of `grp`. The reference program is written for one: setup_inputs(seed, part) draws one part's arguments, and reference() takes and returns one part's arrays. A program takes and returns all parts, laid end to end along the dimension named above; an argument that names none is the same for every part. Nothing has to cross between parts.
Inputs may be any that keep to these rules, and one draw needn't show every extreme that they name: Entries of tokens are finite with scales that vary by row and by column. `select`: row b lists distinct key blocks that start no later than query block b ends, or -1 for an empty slot. Every query block lists each key block of its own index of kv up to its own last position. Apart from its own index, the query blocks of one index of kv together list at most 2 distinct key blocks held by any other index; every index but the first lists exactly 2 blocks of the index before it.
All inputs are finite; a program needn't handle non-finite values.
Results may differ from the reference program's by a relative error of at most 0.012.
Values may be sent and summed in bfloat16 or wider, within the bound.
A program may use at most 128 MiB of HBM per device.

```python
import math
import jax
import jax.numpy as jnp
from jax import lax

D = 2048
HEADS = 8
KV_HEADS = 4
HD = 128
TOK_DEV = 512
QB = 128
KB = 32
NSEL = 32
TOKENS = 2048
NQB = 16
NKB = 64
N_KV = 4


def draw_tokens(key, part):
    base_key = jax.random.fold_in(key, 11)
    draw_keys = jax.random.split(base_key, 3)
    column = jnp.arange(D, dtype=jnp.float32)
    base_draw = jnp.clip(jax.random.normal(draw_keys[0], (TOKENS, D), jnp.float32), -6.0, 6.0)
    rise_factor = 3.0 ** (column / D)
    row_scale = jnp.exp(jax.random.uniform(draw_keys[1], (TOKENS, 1), jnp.float32, 0.0, math.log(10.0)))
    col_scale = jnp.exp(jax.random.uniform(draw_keys[2], (1, D), jnp.float32, 0.0, math.log(10.0)))
    return (base_draw * row_scale * col_scale * rise_factor[None, :]).astype(jnp.bfloat16)


def query_weight(key):
    normal_draw = jax.random.normal(jax.random.fold_in(key, 21), (D, HEADS * HD), jnp.float32)
    return jnp.clip(normal_draw, -6.0, 6.0) / math.sqrt(D)


def draw_w_query(key, part):
    return query_weight(key).astype(jnp.bfloat16)


def draw_w_key(key, part):
    own_part = jnp.clip(jax.random.normal(jax.random.fold_in(key, 22), (D, KV_HEADS * HD), jnp.float32), -6.0, 6.0) / math.sqrt(D)
    own_part = jnp.clip(own_part, -3.0, 3.0)
    return own_part.astype(jnp.bfloat16)


def draw_select(key, part):
    base_key = jax.random.fold_in(key, 31)
    query_blocks = TOK_DEV // QB
    block_ratio = QB // KB
    blocks_dev = TOK_DEV // KB
    owner_ids = jnp.arange(N_KV, dtype=jnp.int32)
    hot_owner = (jax.random.randint(jax.random.fold_in(base_key, 1), (N_KV,), 0, 4) == 0).astype(jnp.int32)
    first_pick = jax.random.randint(jax.random.fold_in(base_key, 2), (N_KV, N_KV), 0, blocks_dev)
    step_offset = jax.random.randint(jax.random.fold_in(base_key, 3), (N_KV, N_KV), 1, blocks_dev)
    second_pick = (first_pick + step_offset) % blocks_dev
    slot_ids = jnp.arange(NSEL, dtype=jnp.int32)

    def draw_row(block_id):
        device = block_id // query_blocks
        local_block = block_id % query_blocks
        own_count = block_ratio * (local_block + 1)
        pair_count = (NSEL - own_count) // 2
        noise_bits = jax.random.randint(jax.random.fold_in(jax.random.fold_in(base_key, 4), block_id), (N_KV,), 0, 1 << 12)
        forced = (owner_ids == device - 1) | (owner_ids == device - N_KV // 2) & (device >= N_KV // 2)
        scores = noise_bits + hot_owner * (1 << 13) + forced.astype(jnp.int32) * (1 << 15)
        scores = jnp.where(owner_ids < device, scores, -(1 << 16))
        scores = scores * N_KV + owner_ids
        ranking = jnp.argsort(-scores, stable=True).astype(jnp.int32)
        rank_ids = jnp.arange(N_KV, dtype=jnp.int32)
        usable = (rank_ids < pair_count) & (ranking < device)
        block_a = ranking * blocks_dev + first_pick[device, ranking]
        block_b = ranking * blocks_dev + second_pick[device, ranking]
        pair_ids = jnp.where(usable[:, None], jnp.stack([block_a, block_b], axis=1), -1).reshape(-1)
        pair_ids = jnp.concatenate([pair_ids, jnp.full((NSEL,), -1, jnp.int32)])
        own_ids = device * blocks_dev + slot_ids
        from_pairs = jnp.take(pair_ids, jnp.maximum(slot_ids - own_count, 0))
        return jnp.where(slot_ids < own_count, own_ids, from_pairs).astype(jnp.int32)
    return jax.vmap(draw_row)(jnp.arange(NQB, dtype=jnp.int32))


def steps_of(key, shape, cuts, smallest, largest):
    level = 1.0
    for position, shards_of in cuts:
        draws = jax.random.uniform(jax.random.fold_in(jax.random.fold_in(key, 6), position), (shards_of,), jnp.float32, smallest / len(cuts), largest / len(cuts))
        level = level * jnp.repeat(jnp.exp(draws), shape[position] // shards_of).reshape((-1,) + (1,) * (len(shape) - 1 - position))
    return level


def scatter_about(key, extent, width, most, shards=(), kind=jnp.bfloat16):
    entries = width * jax.random.normal(key, extent, jnp.float32)
    if shards:
        entries = entries * steps_of(key, extent, shards, -0.22, 0.18)
    return jnp.clip(entries, -most, most).astype(kind)


def setup_inputs(seed: int = 0, part: int = 0) -> dict:
    splits = jax.random.split(jax.random.key(seed), 8)
    part_splits = jax.random.split(jax.random.fold_in(splits[7], part), 8)
    return {
        "tokens": draw_tokens(jax.random.fold_in(jax.random.fold_in(splits[7], part), 71), part),
        "gain": jnp.clip(1.0 + 0.18 * jax.random.normal(splits[1], (D,), jnp.float32), 0.099609375, 1.8984375).astype(jnp.bfloat16),
        "w_query": draw_w_query(jax.random.fold_in(splits[7], 71), part),
        "w_key": draw_w_key(jax.random.fold_in(splits[7], 71), part),
        "w_value": scatter_about(splits[4], (D, KV_HEADS * HD), D ** -0.5, 0.125, ((1, 4),)),
        "w_out": scatter_about(splits[5], (HEADS * HD, D), (max(HEADS * HD // 128, 1)) ** -0.5, 2.0, ((1, 4),)),
        "select": draw_select(jax.random.fold_in(jax.random.fold_in(splits[7], part), 71), part),
    }


epsilon = 1e-06
theta = 10000.0

def rotary(values, positions):
    head_width = values.shape[-1]
    frequency = theta ** (-jnp.arange(0, head_width, 2, dtype=jnp.float32) / head_width)
    angles = positions.astype(jnp.float32)[:, None] * frequency[None, :]
    cosine = jnp.cos(angles)[:, None, :]
    sine_table = jnp.sin(angles)[:, None, :]
    front_half = values[..., :head_width // 2]
    second = values[..., head_width // 2:]
    return jnp.concatenate([front_half * cosine - second * sine_table, second * cosine + front_half * sine_table], axis=-1)

def reference(tokens, gain, w_query, w_key, w_value, w_out, select):
    tokens_f32 = tokens.astype(jnp.float32)
    mean_square = lax.optimization_barrier(jnp.mean(tokens_f32 * tokens_f32, axis=1))
    scaled = (tokens_f32 * gain.astype(jnp.float32)[None, :]).astype(jnp.bfloat16)
    inverse = lax.rsqrt(mean_square + epsilon)[:, None]
    positions = jnp.arange(TOKENS, dtype=jnp.int32)
    query_pre = jnp.dot(scaled, w_query, preferred_element_type=jnp.float32) * inverse
    key_pre = jnp.dot(scaled, w_key, preferred_element_type=jnp.float32) * inverse
    value_pre = jnp.dot(scaled, w_value, preferred_element_type=jnp.float32) * inverse
    queries = rotary(query_pre.reshape(TOKENS, HEADS, HD), positions).astype(jnp.bfloat16)
    keys_all = rotary(key_pre.reshape(TOKENS, KV_HEADS, HD), positions).astype(jnp.bfloat16)
    values_all = value_pre.astype(jnp.bfloat16).reshape(TOKENS, KV_HEADS, HD)
    group_size = HEADS // KV_HEADS
    key_blocks = keys_all.reshape(NKB, KB, KV_HEADS, HD)
    value_blocks = values_all.reshape(NKB, KB, KV_HEADS, HD)

    def one_block(block_id):
        block_ids = select[block_id]
        safe_ids = jnp.maximum(block_ids, 0)
        keys_sel = jnp.take(key_blocks, safe_ids, axis=0).reshape(NSEL * KB, KV_HEADS, HD).astype(jnp.float32)
        values_sel = jnp.take(value_blocks, safe_ids, axis=0).reshape(NSEL * KB, KV_HEADS, HD).astype(jnp.float32)
        query_rows = lax.dynamic_slice_in_dim(queries, block_id * QB, QB, 0)
        query_rows = query_rows.reshape(QB, KV_HEADS, group_size, HD).astype(jnp.float32)
        scores = jnp.einsum('qgrd,kgd->grqk', query_rows, keys_sel) * HD ** (-0.5)
        key_pos = (safe_ids[:, None] * KB + jnp.arange(KB, dtype=jnp.int32)[None, :]).reshape(-1)
        live_keys = jnp.repeat(block_ids >= 0, KB)
        q_pos = block_id * QB + jnp.arange(QB, dtype=jnp.int32)
        allowed = live_keys[None, :] & (key_pos[None, :] <= q_pos[:, None])
        scores = jnp.where(allowed[None, None], scores, -jnp.inf)
        row_max = lax.optimization_barrier(jnp.max(scores, axis=-1, keepdims=True))
        raised = jnp.exp(scores - row_max)
        weights = (raised / lax.optimization_barrier(jnp.sum(raised, axis=-1, keepdims=True))).astype(jnp.bfloat16)
        attended = jnp.einsum('grqk,kgd->qgrd', weights.astype(jnp.float32), values_sel)
        return attended.astype(jnp.bfloat16).reshape(QB, HEADS * HD)
    attended_all = lax.map(one_block, jnp.arange(NQB, dtype=jnp.int32)).reshape(TOKENS, HEADS * HD)
    return jnp.dot(attended_all, w_out, preferred_element_type=jnp.float32).astype(jnp.bfloat16)
```

```python
import functools

import jax
import jax.numpy as jnp
from jax import lax
from jax.experimental import pallas as pl
from jax.experimental.pallas import tpu as pltpu
from jax.sharding import PartitionSpec as P

HD = 128
QB = 128
KB = 32
CAP = 2

epsilon = 1e-06
theta = 10000.0
MESH = pl.DeviceIdType.MESH
F32 = jnp.float32
BF16 = jnp.bfloat16
LOW = -1e30


def loop(count, body):
    if count <= 4:
        for i in range(count):
            body(i)
    else:
        lax.fori_loop(0, count, lambda i, c: (body(i), c)[1], 0)


def kernel(
    tp, n_kv,
    tokens, gain, w_query, w_key, w_value, w_out, select,
    out,
    tok, att, w_in, w_o, q_s, kv_s, hot_s, cos_s, sin_s, o_s, m_s, l_s,
    sel_all, send_kv, recv_kv, bias_s,
    local_sem, tok_send, tok_recv, fwd_send, fwd_recv, mate_send, mate_recv,
    sel_send, sel_recv, kv_send, kv_recv,
    att_send, att_recv, afwd_send, afwd_recv, amate_send, amate_recv,
):
    rows, cols = tokens.shape
    width = tp * cols
    blocks = rows // QB
    groups = tp // 2
    me_tp = lax.axis_index("tp")
    me_kv = lax.axis_index("kv")
    side = lax.rem(me_tp, 2)
    group = lax.div(me_tp, 2)
    mate = group * 2 + 1 - side
    nq, nk = w_query.shape[1], w_key.shape[1]
    heads, kv_heads = nq // HD, nk // HD
    per = heads // kv_heads
    dev_blocks = rows // KB
    spec_rows = CAP * KB

    def other(i):
        return lax.rem(group + 1 + i, groups) * 2 + side

    copies = [
        pltpu.make_async_copy(tokens, tok.at[me_tp], local_sem.at[0]),
        pltpu.make_async_copy(w_query, w_in.at[:, pl.ds(0, nq)], local_sem.at[1]),
        pltpu.make_async_copy(w_key, w_in.at[:, pl.ds(nq, nk)], local_sem.at[2]),
        pltpu.make_async_copy(w_value, w_in.at[:, pl.ds(nq + nk, nk)], local_sem.at[3]),
        pltpu.make_async_copy(w_out, w_o, local_sem.at[4]),
    ]
    for copy in copies:
        copy.start()

    barrier = pltpu.get_barrier_semaphore()
    pl.semaphore_signal(barrier, inc=1, device_id={"tp": mate}, device_id_type=MESH)
    for i in range(groups - 1):
        pl.semaphore_signal(barrier, inc=1, device_id={"tp": other(i)}, device_id_type=MESH)

    def greet(i):
        peer = lax.rem(me_kv + 1 + i, n_kv)
        pl.semaphore_signal(barrier, inc=1, device_id={"kv": peer}, device_id_type=MESH)

    loop(n_kv - 1, greet)
    pl.semaphore_wait(barrier, groups + n_kv - 1)

    def piece(ref, slot, b):
        return ref.at[slot, pl.ds(b * QB, QB), :]

    def tok_copy(i, b):
        return pltpu.make_async_remote_copy(
            src_ref=tokens.at[pl.ds(b * QB, QB), :], dst_ref=piece(tok, me_tp, b),
            send_sem=tok_send.at[i, b], recv_sem=tok_recv.at[groups - 2 - i, b],
            device_id={"tp": other(i)}, device_id_type=MESH)

    def tok_wait(i, b):
        return pltpu.make_async_remote_copy(
            src_ref=tokens.at[pl.ds(b * QB, QB), :], dst_ref=piece(tok, other(i), b),
            send_sem=tok_send.at[i, b], recv_sem=tok_recv.at[i, b],
            device_id={"tp": other(i)}, device_id_type=MESH)

    def mate_copy(b):
        return pltpu.make_async_remote_copy(
            src_ref=tokens.at[pl.ds(b * QB, QB), :], dst_ref=piece(tok, me_tp, b),
            send_sem=mate_send.at[b], recv_sem=mate_recv.at[b],
            device_id={"tp": mate}, device_id_type=MESH)

    def fwd_copy(i, b):
        return pltpu.make_async_remote_copy(
            src_ref=piece(tok, other(i), b), dst_ref=piece(tok, other(i), b),
            send_sem=fwd_send.at[i, b], recv_sem=fwd_recv.at[i, b],
            device_id={"tp": mate}, device_id_type=MESH)

    for b in range(blocks):
        for i in range(groups - 1):
            tok_copy(i, b).start()
        mate_copy(b).start()

    def sel_copy(peer):
        return pltpu.make_async_remote_copy(
            src_ref=select, dst_ref=sel_all.at[me_kv],
            send_sem=sel_send.at[peer], recv_sem=sel_recv.at[me_kv],
            device_id={"kv": peer}, device_id_type=MESH)

    def sel_wait(peer):
        return pltpu.make_async_remote_copy(
            src_ref=select, dst_ref=sel_all.at[peer],
            send_sem=sel_send.at[peer], recv_sem=sel_recv.at[peer],
            device_id={"kv": peer}, device_id_type=MESH)

    def send_select(peer):
        @pl.when(peer < me_kv)
        def _():
            sel_copy(peer).start()

    loop(n_kv - 1, send_select)

    lane = lax.broadcasted_iota(jnp.int32, (1, HD), 1)
    half = HD // 2
    frequency = jnp.exp(
        lax.rem(lane, half).astype(F32) * (-2.0 / HD) * jnp.log(F32(theta)))
    for b in range(blocks):
        place = me_kv * rows + b * QB + lax.broadcasted_iota(jnp.int32, (QB, HD), 0)
        angle = place.astype(F32) * frequency
        cos_s[b * QB:(b + 1) * QB, :] = jnp.cos(angle)
        sine = jnp.sin(angle)
        sin_s[b * QB:(b + 1) * QB, :] = jnp.where(lane < half, -sine, sine)

    chunks, chunk_owners, chunk_keys = bias_s.shape[0], recv_kv.shape[1], bias_s.shape[2]
    listed = select[...]

    def bounds(ids, owner):
        first = owner * dev_blocks
        inside = (ids >= first) & (ids < first + dev_blocks)
        low = jnp.min(jnp.where(inside, ids, 1 << 20), axis=(0, 1), keepdims=True)
        high = jnp.max(jnp.where(inside, ids, -1), axis=(0, 1), keepdims=True)
        return low, high

    key_lane = lax.broadcasted_iota(jnp.int32, (1, chunk_keys), 1)

    def make_bias(c):
        bias = jnp.full((blocks, chunk_keys), LOW, F32)
        for w in range(chunk_owners):
            owner = c * chunk_owners + w
            low, high = bounds(listed, owner)
            has_low = jnp.max(jnp.where(listed == low, 1, 0), axis=1, keepdims=True)
            has_high = jnp.max(
                jnp.where((listed == high) & (high > low), 1, 0), axis=1, keepdims=True)
            start = w * spec_rows
            in_low = (key_lane >= start) & (key_lane < start + KB)
            in_high = (key_lane >= start + KB) & (key_lane < start + spec_rows)
            hit = jnp.where(in_low, has_low, 0) + jnp.where(in_high, has_high, 0)
            hit = jnp.where(owner < me_kv, hit, 0)
            bias = jnp.where(hit > 0, 0.0, bias)

            @pl.when(owner >= me_kv)
            def _():
                recv_kv[c, w] = jnp.zeros(recv_kv.shape[2:], recv_kv.dtype)

        bias_s[c] = bias

    loop(chunks, make_bias)

    def make_hot(p):
        peer = p + 1

        @pl.when(peer > me_kv)
        def _():
            sel_wait(peer).wait_recv()
            low, high = bounds(sel_all[peer], me_kv)
            row = lax.broadcasted_iota(jnp.int32, (spec_rows, 1), 0)
            want = jnp.where(row < KB, low, high) * KB + lax.rem(row, KB) - me_kv * rows
            col = lax.broadcasted_iota(jnp.int32, (spec_rows, rows), 1)
            hot_s[peer] = jnp.where(col == want, 1.0, 0.0).astype(BF16)

    loop(n_kv - 1, make_hot)

    for copy in copies[:4]:
        copy.wait()

    def add_part(slot, b, acc, squares):
        part = tok[slot, pl.ds(b * QB, QB), :].astype(F32)
        factor = gain[:, pl.ds(pl.multiple_of(slot * cols, cols), cols)].astype(F32)
        scaled = (part * factor).astype(BF16)
        weight = w_in[pl.ds(pl.multiple_of(slot * cols, cols), cols), :]
        acc = acc + jnp.dot(scaled, weight, preferred_element_type=F32)
        squares = squares + jnp.sum(part * part, axis=1, keepdims=True)
        return acc, squares

    def rotate(x, b):
        cosine = cos_s[b * QB:(b + 1) * QB, :]
        sine = sin_s[b * QB:(b + 1) * QB, :]
        return x * cosine + pltpu.roll(x, half, 1) * sine

    factor2 = HD ** (-0.5) * 1.4426950408889634

    def project(b):
        acc = jnp.zeros((QB, nq + 2 * nk), F32)
        squares = jnp.zeros((QB, 1), F32)
        acc, squares = add_part(me_tp, b, acc, squares)
        mate_copy(b).wait_recv()
        acc, squares = add_part(mate, b, acc, squares)
        for i in range(groups - 1):
            tok_wait(i, b).wait_recv()
            fwd_copy(i, b).start()
            acc, squares = add_part(other(i), b, acc, squares)
        for i in range(groups - 1):
            fwd_copy(i, b).wait_recv()
            far = lax.rem(group + 1 + i, groups) * 2 + 1 - side
            acc, squares = add_part(far, b, acc, squares)
        inverse = lax.rsqrt(squares / width + epsilon)
        acc = acc * inverse
        here = slice(b * QB, (b + 1) * QB)
        for h in range(heads):
            q_s[h, here, :] = rotate(acc[:, h * HD:(h + 1) * HD], b).astype(BF16)
        for g in range(kv_heads):
            at = nq + g * HD
            kv_s[here, g * HD:(g + 1) * HD] = rotate(acc[:, at:at + HD], b).astype(BF16)
        kv_s[here, nk:] = acc[:, nq + nk:].astype(BF16)

    def head_rows(b, g):
        parts = [q_s[g * per + r, b * QB:(b + 1) * QB, :] for r in range(per)]
        return jnp.concatenate(parts, axis=0)

    def near(b):
        count = (b + 1) * QB
        for g in range(kv_heads):
            here = slice(g * HD, (g + 1) * HD)
            there = slice(nk + g * HD, nk + (g + 1) * HD)
            scores = lax.dot_general(
                head_rows(b, g), kv_s[0:count, here], (((1,), (1,)), ((), ())),
                preferred_element_type=F32) * factor2
            row = lax.rem(lax.broadcasted_iota(jnp.int32, scores.shape, 0), QB) + b * QB
            col = lax.broadcasted_iota(jnp.int32, scores.shape, 1)
            scores = jnp.where(col <= row, scores, LOW)
            top = jnp.max(scores, axis=1, keepdims=True)
            raised = jnp.exp2(scores - top)
            m_s[b, g] = jnp.broadcast_to(top, m_s.shape[2:])
            l_s[b, g] = jnp.broadcast_to(jnp.sum(raised, axis=1, keepdims=True), l_s.shape[2:])
            o_s[b, g] = jnp.dot(
                raised.astype(BF16), kv_s[0:count, there], preferred_element_type=F32)

    def add_far(c, b):
        for g in range(kv_heads):
            here = slice(g * HD, (g + 1) * HD)
            there = slice(nk + g * HD, nk + (g + 1) * HD)
            far_k = jnp.concatenate(
                [recv_kv[c, w, :, here] for w in range(chunk_owners)], axis=0)
            far_v = jnp.concatenate(
                [recv_kv[c, w, :, there] for w in range(chunk_owners)], axis=0)
            scores = lax.dot_general(
                head_rows(b, g), far_k, (((1,), (1,)), ((), ())),
                preferred_element_type=F32) * factor2
            hit = bias_s[c, b:b + 1, :] == 0.0
            scores = jnp.where(hit, scores, LOW)
            before = m_s[b, g]
            top = jnp.maximum(before, jnp.max(scores, axis=1, keepdims=True))
            keep = jnp.exp2(before - top)
            raised = jnp.exp2(scores - top[:, 0:1])
            m_s[b, g] = top
            l_s[b, g] = l_s[b, g] * keep + jnp.sum(raised, axis=1, keepdims=True)
            o_s[b, g] = o_s[b, g] * keep + jnp.dot(
                raised.astype(BF16), far_v, preferred_element_type=F32)

    def kv_copy(peer):
        return pltpu.make_async_remote_copy(
            src_ref=send_kv.at[peer],
            dst_ref=recv_kv.at[lax.div(me_kv, chunk_owners), lax.rem(me_kv, chunk_owners)],
            send_sem=kv_send.at[peer], recv_sem=kv_recv.at[me_kv],
            device_id={"kv": peer}, device_id_type=MESH)

    def kv_wait(peer):
        return pltpu.make_async_remote_copy(
            src_ref=send_kv.at[peer],
            dst_ref=recv_kv.at[lax.div(peer, chunk_owners), lax.rem(peer, chunk_owners)],
            send_sem=kv_send.at[peer], recv_sem=kv_recv.at[peer],
            device_id={"kv": peer}, device_id_type=MESH)

    def send_blocks(p):
        peer = p + 1

        @pl.when(peer > me_kv)
        def _():
            send_kv[peer] = jnp.dot(
                hot_s[peer], kv_s[...], preferred_element_type=F32).astype(BF16)
            kv_copy(peer).start()

    for b in range(blocks):
        project(b)
        if b == blocks - 1:
            loop(n_kv - 1, send_blocks)
        near(b)

    def take_blocks(peer):
        @pl.when(peer < me_kv)
        def _():
            kv_wait(peer).wait_recv()

    loop(n_kv - 1, take_blocks)
    copies[4].wait()

    def att_copy(i, b):
        return pltpu.make_async_remote_copy(
            src_ref=piece(att, me_tp, b), dst_ref=piece(att, me_tp, b),
            send_sem=att_send.at[i, b], recv_sem=att_recv.at[groups - 2 - i, b],
            device_id={"tp": other(i)}, device_id_type=MESH)

    def att_wait(i, b):
        return pltpu.make_async_remote_copy(
            src_ref=piece(att, me_tp, b), dst_ref=piece(att, other(i), b),
            send_sem=att_send.at[i, b], recv_sem=att_recv.at[i, b],
            device_id={"tp": other(i)}, device_id_type=MESH)

    def amate_copy(b):
        return pltpu.make_async_remote_copy(
            src_ref=piece(att, me_tp, b), dst_ref=piece(att, me_tp, b),
            send_sem=amate_send.at[b], recv_sem=amate_recv.at[b],
            device_id={"tp": mate}, device_id_type=MESH)

    def amate_wait(b):
        return pltpu.make_async_remote_copy(
            src_ref=piece(att, me_tp, b), dst_ref=piece(att, mate, b),
            send_sem=amate_send.at[b], recv_sem=amate_recv.at[b],
            device_id={"tp": mate}, device_id_type=MESH)

    def afwd_copy(i, b):
        return pltpu.make_async_remote_copy(
            src_ref=piece(att, other(i), b), dst_ref=piece(att, other(i), b),
            send_sem=afwd_send.at[i, b], recv_sem=afwd_recv.at[i, b],
            device_id={"tp": mate}, device_id_type=MESH)

    for b in range(blocks):
        loop(chunks, functools.partial(add_far, b=b))
        for g in range(kv_heads):
            done = (o_s[b, g] / l_s[b, g]).astype(BF16)
            for r in range(per):
                h = g * per + r
                att[me_tp, pl.ds(b * QB, QB), h * HD:(h + 1) * HD] = (
                    done[r * QB:(r + 1) * QB])
        for i in range(groups - 1):
            att_copy(i, b).start()
        amate_copy(b).start()

    def mix(slot, b):
        weight = w_o[pl.ds(pl.multiple_of(slot * nq, nq), nq), :]
        return jnp.dot(att[slot, pl.ds(b * QB, QB), :], weight, preferred_element_type=F32)

    def relay(b):
        for i in range(groups - 1):
            att_wait(i, b).wait_recv()
            afwd_copy(i, b).start()

    relay(0)
    for b in range(blocks):
        amate_wait(b).wait_recv()
        total = mix(me_tp, b) + mix(mate, b)
        for i in range(groups - 1):
            total = total + mix(other(i), b)
        if b + 1 < blocks:
            relay(b + 1)
        for i in range(groups - 1):
            afwd_copy(i, b).wait_recv()
            far = lax.rem(group + 1 + i, groups) * 2 + 1 - side
            total = total + mix(far, b)
        out[b * QB:(b + 1) * QB, :] = total.astype(out.dtype)

    for b in range(blocks):
        mate_copy(b).wait_send()
        amate_copy(b).wait_send()
        for i in range(groups - 1):
            tok_copy(i, b).wait_send()
            fwd_copy(i, b).wait_send()
            att_copy(i, b).wait_send()
            afwd_copy(i, b).wait_send()

    def finish(p):
        @pl.when(p < me_kv)
        def _():
            sel_copy(p).wait_send()

        @pl.when(p + 1 > me_kv)
        def _():
            kv_copy(p + 1).wait_send()

    loop(n_kv - 1, finish)


def per_device(tp, n_kv, tokens, gain, w_query, w_key, w_value, w_out, select):
    rows, cols = tokens.shape
    depth, nq = w_query.shape
    nk = w_key.shape[1]
    heads, kv_heads = nq // HD, nk // HD
    per = heads // kv_heads
    blocks = rows // QB
    groups = tp // 2
    owners = n_kv - 1
    chunk_owners = max(c for c in (1, 2, 3, 4) if owners % c == 0)
    chunks = owners // chunk_owners
    spec_rows = CAP * KB
    dma = pltpu.SemaphoreType.DMA
    anywhere = pl.BlockSpec(memory_space=pl.ANY)
    fast = pl.BlockSpec(memory_space=pltpu.VMEM)
    return pl.pallas_call(
        functools.partial(kernel, tp, n_kv),
        out_shape=jax.ShapeDtypeStruct((rows, w_out.shape[1]), jnp.bfloat16),
        in_specs=[anywhere, fast, anywhere, anywhere, anywhere, anywhere, fast],
        out_specs=fast,
        scratch_shapes=[
            pltpu.VMEM((tp, rows, cols), BF16),
            pltpu.VMEM((tp, rows, nq), BF16),
            pltpu.VMEM((depth, nq + 2 * nk), BF16),
            pltpu.VMEM(w_out.shape, BF16),
            pltpu.VMEM((heads, rows, HD), BF16),
            pltpu.VMEM((rows, 2 * nk), BF16),
            pltpu.VMEM((n_kv, spec_rows, rows), BF16),
            pltpu.VMEM((rows, HD), F32),
            pltpu.VMEM((rows, HD), F32),
            pltpu.VMEM((blocks, kv_heads, per * QB, HD), F32),
            pltpu.VMEM((blocks, kv_heads, per * QB, HD), F32),
            pltpu.VMEM((blocks, kv_heads, per * QB, HD), F32),
            pltpu.VMEM((n_kv,) + select.shape, jnp.int32),
            pltpu.VMEM((n_kv, spec_rows, 2 * nk), BF16),
            pltpu.VMEM((chunks, chunk_owners, spec_rows, 2 * nk), BF16),
            pltpu.VMEM((chunks, blocks, chunk_owners * spec_rows), F32),
            dma((5,)),
            dma((groups - 1, blocks)),
            dma((groups - 1, blocks)),
            dma((groups - 1, blocks)),
            dma((groups - 1, blocks)),
            dma((blocks,)),
            dma((blocks,)),
            dma((n_kv,)),
            dma((n_kv,)),
            dma((n_kv,)),
            dma((n_kv,)),
            dma((groups - 1, blocks)),
            dma((groups - 1, blocks)),
            dma((groups - 1, blocks)),
            dma((groups - 1, blocks)),
            dma((blocks,)),
            dma((blocks,)),
        ],
        compiler_params=pltpu.CompilerParams(
            collective_id=0, has_side_effects=True, vmem_limit_bytes=60 * 1024 * 1024),
    )(tokens, gain.reshape(1, -1), w_query, w_key, w_value, w_out, select)


def solution(mesh):
    placed = (
        P(("grp", "kv"), "tp"),
        P(),
        P(None, "tp"),
        P(None, "tp"),
        P(None, "tp"),
        P(None, "tp"),
        P(("grp", "kv"), None),
    )
    return jax.shard_map(
        functools.partial(per_device, mesh.shape["tp"], mesh.shape["kv"]),
        mesh=mesh, in_specs=placed, out_specs=P(("grp", "kv"), "tp"), check_vma=False
    )
```

```python
import functools

import jax
import jax.numpy as jnp
from jax import lax
from jax.experimental import pallas as pl
from jax.experimental.pallas import tpu as pltpu
from jax.sharding import PartitionSpec as P

HD = 128
QB = 128
KB = 32
CAP = 2

epsilon = 1e-06
theta = 10000.0
MESH = pl.DeviceIdType.MESH
F32 = jnp.float32
BF16 = jnp.bfloat16
LOW = -1e30


def loop(count, body):
    if count <= 4:
        for i in range(count):
            body(i)
    else:
        lax.fori_loop(0, count, lambda i, c: (body(i), c)[1], 0)


def kernel(
    tp, n_kv,
    tokens, gain_in, w_query, w_key, w_value, w_out, select_in,
    out,
    gain, select,    tok, att, w_in, w_o, q_s, kv_s, hot_s, cos_s, sin_s, o_s, m_s, l_s,
    sel_all, send_kv, recv_kv, bias_s,
    local_sem, tok_send, tok_recv, fwd_send, fwd_recv, mate_send, mate_recv,
    sel_send, sel_recv, chain_sem, kv_send, kv_recv,
    att_send, att_recv, afwd_send, afwd_recv, amate_send, amate_recv,
):
    rows, cols = tokens.shape
    width = tp * cols
    blocks = rows // QB
    groups = tp // 2
    me_tp = lax.axis_index("tp")
    me_kv = lax.axis_index("kv")
    side = lax.rem(me_tp, 2)
    group = lax.div(me_tp, 2)
    mate = group * 2 + 1 - side
    nq, nk = w_query.shape[1], w_key.shape[1]
    heads, kv_heads = nq // HD, nk // HD
    per = heads // kv_heads
    dev_blocks = rows // KB
    spec_rows = CAP * KB

    def other(i):
        return lax.rem(group + 1 + i, groups) * 2 + side

    copies = [
        pltpu.make_async_copy(tokens, tok.at[me_tp], local_sem.at[0]),
        pltpu.make_async_copy(w_query, w_in.at[:, pl.ds(0, nq)], local_sem.at[1]),
        pltpu.make_async_copy(w_key, w_in.at[:, pl.ds(nq, nk)], local_sem.at[2]),
        pltpu.make_async_copy(w_value, w_in.at[:, pl.ds(nq + nk, nk)], local_sem.at[3]),
        pltpu.make_async_copy(w_out, w_o, local_sem.at[4]),
        pltpu.make_async_copy(gain_in, gain, local_sem.at[5]),
        pltpu.make_async_copy(select_in, select, local_sem.at[6]),
    ]
    for copy in copies:
        copy.start()

    barrier = pltpu.get_barrier_semaphore()
    pl.semaphore_signal(barrier, inc=1, device_id={"tp": mate}, device_id_type=MESH)
    for i in range(groups - 1):
        pl.semaphore_signal(barrier, inc=1, device_id={"tp": other(i)}, device_id_type=MESH)

    @pl.when(me_kv > 0)
    def _():
        pl.semaphore_signal(barrier, inc=1, device_id={"kv": me_kv - 1}, device_id_type=MESH)

    @pl.when(me_kv < n_kv - 1)
    def _():
        pl.semaphore_wait(barrier, groups + 1)

    @pl.when(me_kv == n_kv - 1)
    def _():
        pl.semaphore_wait(barrier, groups)

    def piece(ref, slot, b):
        return ref.at[slot, pl.ds(b * QB, QB), :]

    def tok_copy(i, b):
        return pltpu.make_async_remote_copy(
            src_ref=tokens.at[pl.ds(b * QB, QB), :], dst_ref=piece(tok, me_tp, b),
            send_sem=tok_send.at[i, b], recv_sem=tok_recv.at[groups - 2 - i, b],
            device_id={"tp": other(i)}, device_id_type=MESH)

    def tok_wait(i, b):
        return pltpu.make_async_remote_copy(
            src_ref=tokens.at[pl.ds(b * QB, QB), :], dst_ref=piece(tok, other(i), b),
            send_sem=tok_send.at[i, b], recv_sem=tok_recv.at[i, b],
            device_id={"tp": other(i)}, device_id_type=MESH)

    def mate_copy(b):
        return pltpu.make_async_remote_copy(
            src_ref=tokens.at[pl.ds(b * QB, QB), :], dst_ref=piece(tok, me_tp, b),
            send_sem=mate_send.at[b], recv_sem=mate_recv.at[b],
            device_id={"tp": mate}, device_id_type=MESH)

    def fwd_copy(i, b):
        return pltpu.make_async_remote_copy(
            src_ref=piece(tok, other(i), b), dst_ref=piece(tok, other(i), b),
            send_sem=fwd_send.at[i, b], recv_sem=fwd_recv.at[i, b],
            device_id={"tp": mate}, device_id_type=MESH)

    for b in range(blocks):
        for i in range(groups - 1):
            tok_copy(i, b).start()
        mate_copy(b).start()

    @pl.when(me_kv > 0)
    def _():
        pl.semaphore_wait(chain_sem, 1)

    @pl.when(me_kv < n_kv - 1)
    def _():
        pl.semaphore_signal(
            chain_sem, inc=1, device_id={"kv": me_kv + 1}, device_id_type=MESH)

    def sel_copy(peer):
        return pltpu.make_async_remote_copy(
            src_ref=select_in, dst_ref=sel_all.at[me_kv],
            send_sem=sel_send.at[peer], recv_sem=sel_recv.at[me_kv],
            device_id={"kv": peer}, device_id_type=MESH)

    def sel_wait(peer):
        return pltpu.make_async_remote_copy(
            src_ref=select_in, dst_ref=sel_all.at[peer],
            send_sem=sel_send.at[peer], recv_sem=sel_recv.at[peer],
            device_id={"kv": peer}, device_id_type=MESH)

    def send_select(peer):
        @pl.when(peer < me_kv)
        def _():
            sel_copy(peer).start()

    loop(n_kv - 1, send_select)

    lane = lax.broadcasted_iota(jnp.int32, (1, HD), 1)
    half = HD // 2
    frequency = jnp.exp(
        lax.rem(lane, half).astype(F32) * (-2.0 / HD) * jnp.log(F32(theta)))
    for b in range(blocks):
        place = me_kv * rows + b * QB + lax.broadcasted_iota(jnp.int32, (QB, HD), 0)
        angle = place.astype(F32) * frequency
        cos_s[b * QB:(b + 1) * QB, :] = jnp.cos(angle)
        sine = jnp.sin(angle)
        sin_s[b * QB:(b + 1) * QB, :] = jnp.where(lane < half, -sine, sine)

    chunks, chunk_owners, chunk_keys = bias_s.shape[0], recv_kv.shape[1], bias_s.shape[2]
    copies[6].wait()
    listed = select[...]

    def bounds(ids, owner):
        first = owner * dev_blocks
        inside = (ids >= first) & (ids < first + dev_blocks)
        low = jnp.min(jnp.where(inside, ids, 1 << 20), axis=(0, 1), keepdims=True)
        high = jnp.max(jnp.where(inside, ids, -1), axis=(0, 1), keepdims=True)
        return low, high

    key_lane = lax.broadcasted_iota(jnp.int32, (1, chunk_keys), 1)

    def make_bias(c):
        bias = jnp.full((blocks, chunk_keys), LOW, F32)
        for w in range(chunk_owners):
            owner = c * chunk_owners + w
            low, high = bounds(listed, owner)
            has_low = jnp.max(jnp.where(listed == low, 1, 0), axis=1, keepdims=True)
            has_high = jnp.max(
                jnp.where((listed == high) & (high > low), 1, 0), axis=1, keepdims=True)
            start = w * spec_rows
            in_low = (key_lane >= start) & (key_lane < start + KB)
            in_high = (key_lane >= start + KB) & (key_lane < start + spec_rows)
            hit = jnp.where(in_low, has_low, 0) + jnp.where(in_high, has_high, 0)
            hit = jnp.where(owner < me_kv, hit, 0)
            bias = jnp.where(hit > 0, 0.0, bias)

            @pl.when(owner >= me_kv)
            def _():
                recv_kv[c, w] = jnp.zeros(recv_kv.shape[2:], recv_kv.dtype)

        bias_s[c] = bias

    loop(chunks, make_bias)

    def make_hot(p):
        peer = p + 1

        @pl.when(peer > me_kv)
        def _():
            sel_wait(peer).wait_recv()
            low, high = bounds(sel_all[peer], me_kv)
            row = lax.broadcasted_iota(jnp.int32, (spec_rows, 1), 0)
            want = jnp.where(row < KB, low, high) * KB + lax.rem(row, KB) - me_kv * rows
            col = lax.broadcasted_iota(jnp.int32, (spec_rows, rows), 1)
            hot_s[peer] = jnp.where(col == want, 1.0, 0.0).astype(BF16)

    loop(n_kv - 1, make_hot)

    copies[5].wait()
    for copy in copies[:4]:
        copy.wait()

    def add_part(slot, b, acc, squares):
        part = tok[slot, pl.ds(b * QB, QB), :].astype(F32)
        factor = gain[pl.ds(pl.multiple_of(slot * cols, cols), cols)].astype(F32)[None, :]
        scaled = (part * factor).astype(BF16)
        weight = w_in[pl.ds(pl.multiple_of(slot * cols, cols), cols), :]
        acc = acc + jnp.dot(scaled, weight, preferred_element_type=F32)
        squares = squares + jnp.sum(part * part, axis=1, keepdims=True)
        return acc, squares

    def rotate(x, b):
        cosine = cos_s[b * QB:(b + 1) * QB, :]
        sine = sin_s[b * QB:(b + 1) * QB, :]
        return x * cosine + pltpu.roll(x, half, 1) * sine

    factor2 = HD ** (-0.5) * 1.4426950408889634

    def project(b):
        acc = jnp.zeros((QB, nq + 2 * nk), F32)
        squares = jnp.zeros((QB, 1), F32)
        acc, squares = add_part(me_tp, b, acc, squares)
        mate_copy(b).wait_recv()
        acc, squares = add_part(mate, b, acc, squares)
        for i in range(groups - 1):
            tok_wait(i, b).wait_recv()
            fwd_copy(i, b).start()
            acc, squares = add_part(other(i), b, acc, squares)
        for i in range(groups - 1):
            fwd_copy(i, b).wait_recv()
            far = lax.rem(group + 1 + i, groups) * 2 + 1 - side
            acc, squares = add_part(far, b, acc, squares)
        inverse = lax.rsqrt(squares / width + epsilon)
        acc = acc * inverse
        here = slice(b * QB, (b + 1) * QB)
        for h in range(heads):
            q_s[h, here, :] = rotate(acc[:, h * HD:(h + 1) * HD], b).astype(BF16)
        for g in range(kv_heads):
            at = nq + g * HD
            kv_s[here, g * HD:(g + 1) * HD] = rotate(acc[:, at:at + HD], b).astype(BF16)
        kv_s[here, nk:] = acc[:, nq + nk:].astype(BF16)

    def head_rows(b, g):
        parts = [q_s[g * per + r, b * QB:(b + 1) * QB, :] for r in range(per)]
        return jnp.concatenate(parts, axis=0)

    def near(b):
        count = (b + 1) * QB
        for g in range(kv_heads):
            here = slice(g * HD, (g + 1) * HD)
            there = slice(nk + g * HD, nk + (g + 1) * HD)
            scores = lax.dot_general(
                head_rows(b, g), kv_s[0:count, here], (((1,), (1,)), ((), ())),
                preferred_element_type=F32) * factor2
            row = lax.rem(lax.broadcasted_iota(jnp.int32, scores.shape, 0), QB) + b * QB
            col = lax.broadcasted_iota(jnp.int32, scores.shape, 1)
            scores = jnp.where(col <= row, scores, LOW)
            top = jnp.max(scores, axis=1, keepdims=True)
            raised = jnp.exp2(scores - top)
            m_s[b, g] = jnp.broadcast_to(top, m_s.shape[2:])
            l_s[b, g] = jnp.broadcast_to(jnp.sum(raised, axis=1, keepdims=True), l_s.shape[2:])
            o_s[b, g] = jnp.dot(
                raised.astype(BF16), kv_s[0:count, there], preferred_element_type=F32)

    def add_far(c, b):
        for g in range(kv_heads):
            here = slice(g * HD, (g + 1) * HD)
            there = slice(nk + g * HD, nk + (g + 1) * HD)
            far_k = jnp.concatenate(
                [recv_kv[c, w, :, here] for w in range(chunk_owners)], axis=0)
            far_v = jnp.concatenate(
                [recv_kv[c, w, :, there] for w in range(chunk_owners)], axis=0)
            scores = lax.dot_general(
                head_rows(b, g), far_k, (((1,), (1,)), ((), ())),
                preferred_element_type=F32) * factor2
            hit = bias_s[c, b:b + 1, :] == 0.0
            scores = jnp.where(hit, scores, LOW)
            before = m_s[b, g]
            top = jnp.maximum(before, jnp.max(scores, axis=1, keepdims=True))
            keep = jnp.exp2(before - top)
            raised = jnp.exp2(scores - top[:, 0:1])
            m_s[b, g] = top
            l_s[b, g] = l_s[b, g] * keep + jnp.sum(raised, axis=1, keepdims=True)
            o_s[b, g] = o_s[b, g] * keep + jnp.dot(
                raised.astype(BF16), far_v, preferred_element_type=F32)

    def kv_copy(peer):
        return pltpu.make_async_remote_copy(
            src_ref=send_kv.at[peer],
            dst_ref=recv_kv.at[lax.div(me_kv, chunk_owners), lax.rem(me_kv, chunk_owners)],
            send_sem=kv_send.at[peer], recv_sem=kv_recv.at[me_kv],
            device_id={"kv": peer}, device_id_type=MESH)

    def kv_wait(peer):
        return pltpu.make_async_remote_copy(
            src_ref=send_kv.at[peer],
            dst_ref=recv_kv.at[lax.div(peer, chunk_owners), lax.rem(peer, chunk_owners)],
            send_sem=kv_send.at[peer], recv_sem=kv_recv.at[peer],
            device_id={"kv": peer}, device_id_type=MESH)

    def send_blocks(p):
        peer = p + 1

        @pl.when(peer > me_kv)
        def _():
            send_kv[peer] = jnp.dot(
                hot_s[peer], kv_s[...], preferred_element_type=F32).astype(BF16)
            kv_copy(peer).start()

    for b in range(blocks):
        project(b)
        if b == blocks - 1:
            loop(n_kv - 1, send_blocks)
        near(b)

    def take_blocks(peer):
        @pl.when(peer < me_kv)
        def _():
            kv_wait(peer).wait_recv()

    loop(n_kv - 1, take_blocks)
    copies[4].wait()

    def att_copy(i, b):
        return pltpu.make_async_remote_copy(
            src_ref=piece(att, me_tp, b), dst_ref=piece(att, me_tp, b),
            send_sem=att_send.at[i, b], recv_sem=att_recv.at[groups - 2 - i, b],
            device_id={"tp": other(i)}, device_id_type=MESH)

    def att_wait(i, b):
        return pltpu.make_async_remote_copy(
            src_ref=piece(att, me_tp, b), dst_ref=piece(att, other(i), b),
            send_sem=att_send.at[i, b], recv_sem=att_recv.at[i, b],
            device_id={"tp": other(i)}, device_id_type=MESH)

    def amate_copy(b):
        return pltpu.make_async_remote_copy(
            src_ref=piece(att, me_tp, b), dst_ref=piece(att, me_tp, b),
            send_sem=amate_send.at[b], recv_sem=amate_recv.at[b],
            device_id={"tp": mate}, device_id_type=MESH)

    def amate_wait(b):
        return pltpu.make_async_remote_copy(
            src_ref=piece(att, me_tp, b), dst_ref=piece(att, mate, b),
            send_sem=amate_send.at[b], recv_sem=amate_recv.at[b],
            device_id={"tp": mate}, device_id_type=MESH)

    def afwd_copy(i, b):
        return pltpu.make_async_remote_copy(
            src_ref=piece(att, other(i), b), dst_ref=piece(att, other(i), b),
            send_sem=afwd_send.at[i, b], recv_sem=afwd_recv.at[i, b],
            device_id={"tp": mate}, device_id_type=MESH)

    for b in range(blocks):
        loop(chunks, functools.partial(add_far, b=b))
        for g in range(kv_heads):
            done = (o_s[b, g] / l_s[b, g]).astype(BF16)
            for r in range(per):
                h = g * per + r
                att[me_tp, pl.ds(b * QB, QB), h * HD:(h + 1) * HD] = (
                    done[r * QB:(r + 1) * QB])
        for i in range(groups - 1):
            att_copy(i, b).start()
        amate_copy(b).start()

    def mix(slot, b):
        weight = w_o[pl.ds(pl.multiple_of(slot * nq, nq), nq), :]
        return jnp.dot(att[slot, pl.ds(b * QB, QB), :], weight, preferred_element_type=F32)

    def relay(b):
        for i in range(groups - 1):
            att_wait(i, b).wait_recv()
            afwd_copy(i, b).start()

    relay(0)
    for b in range(blocks):
        amate_wait(b).wait_recv()
        total = mix(me_tp, b) + mix(mate, b)
        for i in range(groups - 1):
            total = total + mix(other(i), b)
        if b + 1 < blocks:
            relay(b + 1)
        for i in range(groups - 1):
            afwd_copy(i, b).wait_recv()
            far = lax.rem(group + 1 + i, groups) * 2 + 1 - side
            total = total + mix(far, b)
        out[b * QB:(b + 1) * QB, :] = total.astype(out.dtype)

    for b in range(blocks):
        mate_copy(b).wait_send()
        amate_copy(b).wait_send()
        for i in range(groups - 1):
            tok_copy(i, b).wait_send()
            fwd_copy(i, b).wait_send()
            att_copy(i, b).wait_send()
            afwd_copy(i, b).wait_send()

    def finish(p):
        @pl.when(p < me_kv)
        def _():
            sel_copy(p).wait_send()

        @pl.when(p + 1 > me_kv)
        def _():
            kv_copy(p + 1).wait_send()

    loop(n_kv - 1, finish)


def per_device(tp, n_kv, tokens, gain, w_query, w_key, w_value, w_out, select):
    rows, cols = tokens.shape
    depth, nq = w_query.shape
    nk = w_key.shape[1]
    heads, kv_heads = nq // HD, nk // HD
    per = heads // kv_heads
    blocks = rows // QB
    groups = tp // 2
    owners = n_kv - 1
    chunk_owners = max(c for c in (1, 2, 3, 4) if owners % c == 0)
    chunks = owners // chunk_owners
    spec_rows = CAP * KB
    dma = pltpu.SemaphoreType.DMA
    anywhere = pl.BlockSpec(memory_space=pl.ANY)
    fast = pl.BlockSpec(memory_space=pltpu.VMEM)
    return pl.pallas_call(
        functools.partial(kernel, tp, n_kv),
        out_shape=jax.ShapeDtypeStruct((rows, w_out.shape[1]), jnp.bfloat16),
        in_specs=[anywhere] * 7,
        out_specs=fast,
        scratch_shapes=[
            pltpu.VMEM(gain.shape, BF16),
            pltpu.VMEM(select.shape, jnp.int32),
            pltpu.VMEM((tp, rows, cols), BF16),
            pltpu.VMEM((tp, rows, nq), BF16),
            pltpu.VMEM((depth, nq + 2 * nk), BF16),
            pltpu.VMEM(w_out.shape, BF16),
            pltpu.VMEM((heads, rows, HD), BF16),
            pltpu.VMEM((rows, 2 * nk), BF16),
            pltpu.VMEM((n_kv, spec_rows, rows), BF16),
            pltpu.VMEM((rows, HD), F32),
            pltpu.VMEM((rows, HD), F32),
            pltpu.VMEM((blocks, kv_heads, per * QB, HD), F32),
            pltpu.VMEM((blocks, kv_heads, per * QB, HD), F32),
            pltpu.VMEM((blocks, kv_heads, per * QB, HD), F32),
            pltpu.VMEM((n_kv,) + select.shape, jnp.int32),
            pltpu.VMEM((n_kv, spec_rows, 2 * nk), BF16),
            pltpu.VMEM((chunks, chunk_owners, spec_rows, 2 * nk), BF16),
            pltpu.VMEM((chunks, blocks, chunk_owners * spec_rows), F32),
            dma((7,)),
            dma((groups - 1, blocks)),
            dma((groups - 1, blocks)),
            dma((groups - 1, blocks)),
            dma((groups - 1, blocks)),
            dma((blocks,)),
            dma((blocks,)),
            dma((n_kv,)),
            dma((n_kv,)),
            pltpu.SemaphoreType.REGULAR,
            dma((n_kv,)),
            dma((n_kv,)),
            dma((groups - 1, blocks)),
            dma((groups - 1, blocks)),
            dma((groups - 1, blocks)),
            dma((groups - 1, blocks)),
            dma((blocks,)),
            dma((blocks,)),
        ],
        compiler_params=pltpu.CompilerParams(
            collective_id=0, has_side_effects=True, vmem_limit_bytes=62914560),
    )(tokens, gain, w_query, w_key, w_value, w_out, select)


def solution(mesh):
    placed = (
        P(("grp", "kv"), "tp"),
        P(),
        P(None, "tp"),
        P(None, "tp"),
        P(None, "tp"),
        P(None, "tp"),
        P(("grp", "kv"), None),
    )
    return jax.shard_map(
        functools.partial(per_device, mesh.shape["tp"], mesh.shape["kv"]),
        mesh=mesh, in_specs=placed, out_specs=P(("grp", "kv"), "tp"), check_vma=False
    )
```

```python
import functools

import jax
import jax.numpy as jnp
from jax import lax
from jax.experimental import pallas as pl
from jax.experimental.pallas import tpu as pltpu
from jax.sharding import PartitionSpec as P

HD = 128
QB = 128
KB = 32
CAP = 2

epsilon = 1e-06
theta = 10000.0
MESH = pl.DeviceIdType.MESH
F32 = jnp.float32
BF16 = jnp.bfloat16
LOW = -1e30


def loop(count, body):
    if count <= 4:
        for i in range(count):
            body(i)
    else:
        lax.fori_loop(0, count, lambda i, c: (body(i), c)[1], 0)


def kernel(
    tp, n_kv,
    tokens, gain_in, w_query, w_key, w_value, w_out, select_in,
    out,
    gain, select,    tok, att, w_in, w_o, q_s, kv_s, hot_s, cos_s, sin_s, o_s, m_s, l_s,
    sel_all, send_kv, recv_kv, bias_s,
    local_sem, tok_send, tok_recv, fwd_send, fwd_recv, mate_send, mate_recv,
    sel_send, sel_recv, chain_sem, kv_send, kv_recv,
    att_send, att_recv, afwd_send, afwd_recv, amate_send, amate_recv,
):
    rows, cols = tokens.shape
    width = tp * cols
    blocks = rows // QB
    groups = tp // 2
    me_tp = lax.axis_index("tp")
    me_kv = lax.axis_index("kv")
    side = lax.rem(me_tp, 2)
    group = lax.div(me_tp, 2)
    mate = group * 2 + 1 - side
    nq, nk = w_query.shape[1], w_key.shape[1]
    heads, kv_heads = nq // HD, nk // HD
    per = heads // kv_heads
    dev_blocks = rows // KB
    spec_rows = CAP * KB

    def other(i):
        return lax.rem(group + 1 + i, groups) * 2 + side

    copies = [
        pltpu.make_async_copy(tokens, tok.at[me_tp], local_sem.at[0]),
        pltpu.make_async_copy(w_query, w_in.at[:, pl.ds(0, nq)], local_sem.at[1]),
        pltpu.make_async_copy(w_key, w_in.at[:, pl.ds(nq, nk)], local_sem.at[2]),
        pltpu.make_async_copy(w_value, w_in.at[:, pl.ds(nq + nk, nk)], local_sem.at[3]),
        pltpu.make_async_copy(w_out, w_o, local_sem.at[4]),
        pltpu.make_async_copy(gain_in, gain, local_sem.at[5]),
        pltpu.make_async_copy(select_in, select, local_sem.at[6]),
    ]
    for copy in copies:
        copy.start()

    barrier = pltpu.get_barrier_semaphore()
    pl.semaphore_signal(barrier, inc=1, device_id={"tp": mate}, device_id_type=MESH)
    for i in range(groups - 1):
        pl.semaphore_signal(barrier, inc=1, device_id={"tp": other(i)}, device_id_type=MESH)

    @pl.when(me_kv > 0)
    def _():
        pl.semaphore_signal(barrier, inc=1, device_id={"kv": me_kv - 1}, device_id_type=MESH)

    @pl.when(me_kv < n_kv - 1)
    def _():
        pl.semaphore_wait(barrier, groups + 1)

    @pl.when(me_kv == n_kv - 1)
    def _():
        pl.semaphore_wait(barrier, groups)

    def piece(ref, slot, b):
        return ref.at[slot, pl.ds(b * QB, QB), :]

    def tok_copy(i, b):
        return pltpu.make_async_remote_copy(
            src_ref=tokens.at[pl.ds(b * QB, QB), :], dst_ref=piece(tok, me_tp, b),
            send_sem=tok_send.at[i, b], recv_sem=tok_recv.at[groups - 2 - i, b],
            device_id={"tp": other(i)}, device_id_type=MESH)

    def tok_wait(i, b):
        return pltpu.make_async_remote_copy(
            src_ref=tokens.at[pl.ds(b * QB, QB), :], dst_ref=piece(tok, other(i), b),
            send_sem=tok_send.at[i, b], recv_sem=tok_recv.at[i, b],
            device_id={"tp": other(i)}, device_id_type=MESH)

    def mate_copy(b):
        return pltpu.make_async_remote_copy(
            src_ref=tokens.at[pl.ds(b * QB, QB), :], dst_ref=piece(tok, me_tp, b),
            send_sem=mate_send.at[b], recv_sem=mate_recv.at[b],
            device_id={"tp": mate}, device_id_type=MESH)

    def fwd_copy(i, b):
        return pltpu.make_async_remote_copy(
            src_ref=piece(tok, other(i), b), dst_ref=piece(tok, other(i), b),
            send_sem=fwd_send.at[i, b], recv_sem=fwd_recv.at[i, b],
            device_id={"tp": mate}, device_id_type=MESH)

    for b in range(blocks):
        for i in range(groups - 1):
            tok_copy(i, b).start()
        mate_copy(b).start()

    @pl.when(me_kv > 0)
    def _():
        pl.semaphore_wait(chain_sem, 1)

    @pl.when(me_kv < n_kv - 1)
    def _():
        pl.semaphore_signal(
            chain_sem, inc=1, device_id={"kv": me_kv + 1}, device_id_type=MESH)

    def sel_copy(peer):
        return pltpu.make_async_remote_copy(
            src_ref=select_in, dst_ref=sel_all.at[me_kv],
            send_sem=sel_send.at[peer], recv_sem=sel_recv.at[me_kv],
            device_id={"kv": peer}, device_id_type=MESH)

    def sel_wait(peer):
        return pltpu.make_async_remote_copy(
            src_ref=select_in, dst_ref=sel_all.at[peer],
            send_sem=sel_send.at[peer], recv_sem=sel_recv.at[peer],
            device_id={"kv": peer}, device_id_type=MESH)

    def send_select(peer):
        @pl.when(peer < me_kv)
        def _():
            sel_copy(peer).start()

    loop(n_kv - 1, send_select)

    lane = lax.broadcasted_iota(jnp.int32, (1, HD), 1)
    half = HD // 2
    frequency = jnp.exp(
        lax.rem(lane, half).astype(F32) * (-2.0 / HD) * jnp.log(F32(theta)))
    for b in range(blocks):
        place = me_kv * rows + b * QB + lax.broadcasted_iota(jnp.int32, (QB, HD), 0)
        angle = place.astype(F32) * frequency
        cos_s[b * QB:(b + 1) * QB, :] = jnp.cos(angle)
        sine = jnp.sin(angle)
        sin_s[b * QB:(b + 1) * QB, :] = jnp.where(lane < half, -sine, sine)

    chunks, chunk_owners, chunk_keys = bias_s.shape[0], recv_kv.shape[1], bias_s.shape[2]
    copies[6].wait()
    listed = select[...]

    def bounds(ids, owner):
        first = owner * dev_blocks
        inside = (ids >= first) & (ids < first + dev_blocks)
        low = jnp.min(jnp.where(inside, ids, 1 << 20), axis=(0, 1), keepdims=True)
        high = jnp.max(jnp.where(inside, ids, -1), axis=(0, 1), keepdims=True)
        return low, high

    key_lane = lax.broadcasted_iota(jnp.int32, (1, chunk_keys), 1)

    def make_bias(c):
        bias = jnp.full((blocks, chunk_keys), LOW, F32)
        for w in range(chunk_owners):
            owner = c * chunk_owners + w
            low, high = bounds(listed, owner)
            has_low = jnp.max(jnp.where(listed == low, 1, 0), axis=1, keepdims=True)
            has_high = jnp.max(
                jnp.where((listed == high) & (high > low), 1, 0), axis=1, keepdims=True)
            start = w * spec_rows
            in_low = (key_lane >= start) & (key_lane < start + KB)
            in_high = (key_lane >= start + KB) & (key_lane < start + spec_rows)
            hit = jnp.where(in_low, has_low, 0) + jnp.where(in_high, has_high, 0)
            hit = jnp.where(owner < me_kv, hit, 0)
            bias = jnp.where(hit > 0, 0.0, bias)

            @pl.when(owner >= me_kv)
            def _():
                recv_kv[c, w] = jnp.zeros(recv_kv.shape[2:], recv_kv.dtype)

        bias_s[c] = bias

    loop(chunks, make_bias)

    def make_hot(p):
        peer = p + 1

        @pl.when(peer > me_kv)
        def _():
            sel_wait(peer).wait_recv()
            low, high = bounds(sel_all[peer], me_kv)
            row = lax.broadcasted_iota(jnp.int32, (spec_rows, 1), 0)
            want = jnp.where(row < KB, low, high) * KB + lax.rem(row, KB) - me_kv * rows
            col = lax.broadcasted_iota(jnp.int32, (spec_rows, rows), 1)
            hot_s[peer] = jnp.where(col == want, 1.0, 0.0).astype(BF16)

    loop(n_kv - 1, make_hot)

    copies[5].wait()
    for copy in copies[:4]:
        copy.wait()

    def add_part(slot, b, acc, squares):
        part = tok[slot, pl.ds(b * QB, QB), :].astype(F32)
        factor = gain[pl.ds(pl.multiple_of(slot * cols, cols), cols)].astype(F32)[None, :]
        scaled = (part * factor).astype(BF16)
        weight = w_in[pl.ds(pl.multiple_of(slot * cols, cols), cols), :]
        acc = acc + jnp.dot(scaled, weight, preferred_element_type=F32)
        squares = squares + jnp.sum(part * part, axis=1, keepdims=True)
        return acc, squares

    def rotate(x, b):
        cosine = cos_s[b * QB:(b + 1) * QB, :]
        sine = sin_s[b * QB:(b + 1) * QB, :]
        return x * cosine + pltpu.roll(x, half, 1) * sine

    factor2 = HD ** (-0.5) * 1.4426950408889634

    def project(b):
        acc = jnp.zeros((QB, nq + 2 * nk), F32)
        squares = jnp.zeros((QB, 1), F32)
        acc, squares = add_part(me_tp, b, acc, squares)
        mate_copy(b).wait_recv()
        acc, squares = add_part(mate, b, acc, squares)
        for i in range(groups - 1):
            tok_wait(i, b).wait_recv()
            fwd_copy(i, b).start()
            acc, squares = add_part(other(i), b, acc, squares)
        for i in range(groups - 1):
            fwd_copy(i, b).wait_recv()
            far = lax.rem(group + 1 + i, groups) * 2 + 1 - side
            acc, squares = add_part(far, b, acc, squares)
        inverse = lax.rsqrt(squares / width + epsilon)
        acc = acc * inverse
        here = slice(b * QB, (b + 1) * QB)
        for h in range(heads):
            q_s[h, here, :] = rotate(acc[:, h * HD:(h + 1) * HD], b).astype(BF16)
        for g in range(kv_heads):
            at = nq + g * HD
            kv_s[here, g * HD:(g + 1) * HD] = rotate(acc[:, at:at + HD], b).astype(BF16)
        kv_s[here, nk:] = acc[:, nq + nk:].astype(BF16)

    def head_rows(b, g):
        parts = [q_s[g * per + r, b * QB:(b + 1) * QB, :] for r in range(per)]
        return jnp.concatenate(parts, axis=0)

    def near(b):
        count = (b + 1) * QB
        for g in range(kv_heads):
            here = slice(g * HD, (g + 1) * HD)
            there = slice(nk + g * HD, nk + (g + 1) * HD)
            scores = lax.dot_general(
                head_rows(b, g), kv_s[0:count, here], (((1,), (1,)), ((), ())),
                preferred_element_type=F32) * factor2
            row = lax.rem(lax.broadcasted_iota(jnp.int32, scores.shape, 0), QB) + b * QB
            col = lax.broadcasted_iota(jnp.int32, scores.shape, 1)
            scores = jnp.where(col <= row, scores, LOW)
            top = jnp.max(scores, axis=1, keepdims=True)
            raised = jnp.exp2(scores - top)
            m_s[b, g] = jnp.broadcast_to(top, m_s.shape[2:])
            l_s[b, g] = jnp.broadcast_to(jnp.sum(raised, axis=1, keepdims=True), l_s.shape[2:])
            o_s[b, g] = jnp.dot(
                raised.astype(BF16), kv_s[0:count, there], preferred_element_type=F32)

    def add_far(c, b):
        for g in range(kv_heads):
            here = slice(g * HD, (g + 1) * HD)
            there = slice(nk + g * HD, nk + (g + 1) * HD)
            far_k = jnp.concatenate(
                [recv_kv[c, w, :, here] for w in range(chunk_owners)], axis=0)
            far_v = jnp.concatenate(
                [recv_kv[c, w, :, there] for w in range(chunk_owners)], axis=0)
            scores = lax.dot_general(
                head_rows(b, g), far_k, (((1,), (1,)), ((), ())),
                preferred_element_type=F32) * factor2
            hit = bias_s[c, b:b + 1, :] == 0.0
            scores = jnp.where(hit, scores, LOW)
            before = m_s[b, g]
            top = jnp.maximum(before, jnp.max(scores, axis=1, keepdims=True))
            keep = jnp.exp2(before - top)
            raised = jnp.exp2(scores - top[:, 0:1])
            m_s[b, g] = top
            l_s[b, g] = l_s[b, g] * keep + jnp.sum(raised, axis=1, keepdims=True)
            o_s[b, g] = o_s[b, g] * keep + jnp.dot(
                raised.astype(BF16), far_v, preferred_element_type=F32)

    def kv_copy(peer):
        return pltpu.make_async_remote_copy(
            src_ref=send_kv.at[peer],
            dst_ref=recv_kv.at[lax.div(me_kv, chunk_owners), lax.rem(me_kv, chunk_owners)],
            send_sem=kv_send.at[peer], recv_sem=kv_recv.at[me_kv],
            device_id={"kv": peer}, device_id_type=MESH)

    def kv_wait(peer):
        return pltpu.make_async_remote_copy(
            src_ref=send_kv.at[peer],
            dst_ref=recv_kv.at[lax.div(peer, chunk_owners), lax.rem(peer, chunk_owners)],
            send_sem=kv_send.at[peer], recv_sem=kv_recv.at[peer],
            device_id={"kv": peer}, device_id_type=MESH)

    def send_blocks(p):
        peer = n_kv - 1 - p

        @pl.when(peer > me_kv)
        def _():
            send_kv[peer] = jnp.dot(
                hot_s[peer], kv_s[...], preferred_element_type=F32).astype(BF16)
            kv_copy(peer).start()

    for b in range(blocks):
        project(b)
        if b == blocks - 1:
            loop(n_kv - 1, send_blocks)
        near(b)

    def take_blocks(peer):
        @pl.when(peer < me_kv)
        def _():
            kv_wait(peer).wait_recv()

    loop(n_kv - 1, take_blocks)
    copies[4].wait()

    def att_copy(i, b):
        return pltpu.make_async_remote_copy(
            src_ref=piece(att, me_tp, b), dst_ref=piece(att, me_tp, b),
            send_sem=att_send.at[i, b], recv_sem=att_recv.at[groups - 2 - i, b],
            device_id={"tp": other(i)}, device_id_type=MESH)

    def att_wait(i, b):
        return pltpu.make_async_remote_copy(
            src_ref=piece(att, me_tp, b), dst_ref=piece(att, other(i), b),
            send_sem=att_send.at[i, b], recv_sem=att_recv.at[i, b],
            device_id={"tp": other(i)}, device_id_type=MESH)

    def amate_copy(b):
        return pltpu.make_async_remote_copy(
            src_ref=piece(att, me_tp, b), dst_ref=piece(att, me_tp, b),
            send_sem=amate_send.at[b], recv_sem=amate_recv.at[b],
            device_id={"tp": mate}, device_id_type=MESH)

    def amate_wait(b):
        return pltpu.make_async_remote_copy(
            src_ref=piece(att, me_tp, b), dst_ref=piece(att, mate, b),
            send_sem=amate_send.at[b], recv_sem=amate_recv.at[b],
            device_id={"tp": mate}, device_id_type=MESH)

    def afwd_copy(i, b):
        return pltpu.make_async_remote_copy(
            src_ref=piece(att, other(i), b), dst_ref=piece(att, other(i), b),
            send_sem=afwd_send.at[i, b], recv_sem=afwd_recv.at[i, b],
            device_id={"tp": mate}, device_id_type=MESH)

    for b in range(blocks):
        loop(chunks, functools.partial(add_far, b=b))
        for g in range(kv_heads):
            done = (o_s[b, g] / l_s[b, g]).astype(BF16)
            for r in range(per):
                h = g * per + r
                att[me_tp, pl.ds(b * QB, QB), h * HD:(h + 1) * HD] = (
                    done[r * QB:(r + 1) * QB])
        for i in range(groups - 1):
            att_copy(i, b).start()
        amate_copy(b).start()

    def mix(slot, b):
        weight = w_o[pl.ds(pl.multiple_of(slot * nq, nq), nq), :]
        return jnp.dot(att[slot, pl.ds(b * QB, QB), :], weight, preferred_element_type=F32)

    def relay(b):
        for i in range(groups - 1):
            att_wait(i, b).wait_recv()
            afwd_copy(i, b).start()

    relay(0)
    for b in range(blocks):
        amate_wait(b).wait_recv()
        total = mix(me_tp, b) + mix(mate, b)
        for i in range(groups - 1):
            total = total + mix(other(i), b)
        if b + 1 < blocks:
            relay(b + 1)
        for i in range(groups - 1):
            afwd_copy(i, b).wait_recv()
            far = lax.rem(group + 1 + i, groups) * 2 + 1 - side
            total = total + mix(far, b)
        out[b * QB:(b + 1) * QB, :] = total.astype(out.dtype)

    for b in range(blocks):
        mate_copy(b).wait_send()
        amate_copy(b).wait_send()
        for i in range(groups - 1):
            tok_copy(i, b).wait_send()
            fwd_copy(i, b).wait_send()
            att_copy(i, b).wait_send()
            afwd_copy(i, b).wait_send()

    def finish(p):
        @pl.when(p < me_kv)
        def _():
            sel_copy(p).wait_send()

        @pl.when(p + 1 > me_kv)
        def _():
            kv_copy(p + 1).wait_send()

    loop(n_kv - 1, finish)


def per_device(tp, n_kv, tokens, gain, w_query, w_key, w_value, w_out, select):
    rows, cols = tokens.shape
    depth, nq = w_query.shape
    nk = w_key.shape[1]
    heads, kv_heads = nq // HD, nk // HD
    per = heads // kv_heads
    blocks = rows // QB
    groups = tp // 2
    owners = n_kv - 1
    chunk_owners = max(c for c in (1, 2, 3, 4) if owners % c == 0)
    chunks = owners // chunk_owners
    spec_rows = CAP * KB
    dma = pltpu.SemaphoreType.DMA
    anywhere = pl.BlockSpec(memory_space=pl.ANY)
    fast = pl.BlockSpec(memory_space=pltpu.VMEM)
    return pl.pallas_call(
        functools.partial(kernel, tp, n_kv),
        out_shape=jax.ShapeDtypeStruct((rows, w_out.shape[1]), jnp.bfloat16),
        in_specs=[anywhere] * 7,
        out_specs=fast,
        scratch_shapes=[
            pltpu.VMEM(gain.shape, BF16),
            pltpu.VMEM(select.shape, jnp.int32),
            pltpu.VMEM((tp, rows, cols), BF16),
            pltpu.VMEM((tp, rows, nq), BF16),
            pltpu.VMEM((depth, nq + 2 * nk), BF16),
            pltpu.VMEM(w_out.shape, BF16),
            pltpu.VMEM((heads, rows, HD), BF16),
            pltpu.VMEM((rows, 2 * nk), BF16),
            pltpu.VMEM((n_kv, spec_rows, rows), BF16),
            pltpu.VMEM((rows, HD), F32),
            pltpu.VMEM((rows, HD), F32),
            pltpu.VMEM((blocks, kv_heads, per * QB, HD), F32),
            pltpu.VMEM((blocks, kv_heads, per * QB, HD), F32),
            pltpu.VMEM((blocks, kv_heads, per * QB, HD), F32),
            pltpu.VMEM((n_kv,) + select.shape, jnp.int32),
            pltpu.VMEM((n_kv, spec_rows, 2 * nk), BF16),
            pltpu.VMEM((chunks, chunk_owners, spec_rows, 2 * nk), BF16),
            pltpu.VMEM((chunks, blocks, chunk_owners * spec_rows), F32),
            dma((7,)),
            dma((groups - 1, blocks)),
            dma((groups - 1, blocks)),
            dma((groups - 1, blocks)),
            dma((groups - 1, blocks)),
            dma((blocks,)),
            dma((blocks,)),
            dma((n_kv,)),
            dma((n_kv,)),
            pltpu.SemaphoreType.REGULAR,
            dma((n_kv,)),
            dma((n_kv,)),
            dma((groups - 1, blocks)),
            dma((groups - 1, blocks)),
            dma((groups - 1, blocks)),
            dma((groups - 1, blocks)),
            dma((blocks,)),
            dma((blocks,)),
        ],
        compiler_params=pltpu.CompilerParams(
            collective_id=0, has_side_effects=True, vmem_limit_bytes=54400 * 1024),
    )(tokens, gain, w_query, w_key, w_value, w_out, select)


def solution(mesh):
    placed = (
        P(("grp", "kv"), "tp"),
        P(),
        P(None, "tp"),
        P(None, "tp"),
        P(None, "tp"),
        P(None, "tp"),
        P(("grp", "kv"), None),
    )
    return jax.shard_map(
        functools.partial(per_device, mesh.shape["tp"], mesh.shape["kv"]),
        mesh=mesh, in_specs=placed, out_specs=P(("grp", "kv"), "tp"), check_vma=False
    )
```
